32 devices in a mesh: sp: 16 (over z, y, core), tp: 2 (over x).
Axes of the slice: x: 2, y: 2, z: 4, core: 2. Of those that a mesh axis runs over, the one named last changes fastest.
Arguments:
- tokens: bfloat16 [4096, 2048], P(('sp', 'tp')), may hold values from -6 to 6
- norm_gain: float32 [2048], replicated, may hold values from 0.1 to 1.9
- w_query: bfloat16 [2048, 1024], P('sp', 'tp'), may hold values from -0.125 to 0.125
- w_forget: bfloat16 [2048, 1024], P('sp', 'tp'), may hold values from -0.125 to 0.125
- w_input: bfloat16 [2048, 1024], P('sp', 'tp'), may hold values from -0.125 to 0.125
- w_outgate: bfloat16 [2048, 1024], P('sp', 'tp'), may hold values from -0.125 to 0.125
- w_bgate: bfloat16 [2048, 1024], P('sp', 'tp'), may hold values from -0.125 to 0.125
- w_cgate: bfloat16 [2048, 1024], P('sp', 'tp'), may hold values from -0.125 to 0.125
- w_value: bfloat16 [2048, 1024], P('sp', 'tp'), may hold values from -0.125 to 0.125
- floor_gap: float32 [8, 128], P('tp'), may hold values from 0 to 0.06
- extra_decay: float32 [4096, 8], P('sp', 'tp'), may hold values from -1 to 0
- start_state: float32 [8, 128, 128], P('tp'), may hold values from -0.109375 to 0.109375
- state_gain: float32 [128], replicated, may hold values from 0.1 to 1.9
- conv_taps: float32 [3, 1024], P(None, 'tp'), may hold values from -3 to 3
- out_rec: bfloat16 [1024, 2048], P('tp', 'sp'), may hold values from -0.125 to 0.125
- out_conv: bfloat16 [1024, 2048], P('tp', 'sp'), may hold values from -0.125 to 0.125
Outputs:
- mixed_sum: bfloat16 [4096, 2048], P(('sp', 'tp'))
The draws below stay inside these ranges and needn't reach their ends.
All inputs are finite; a program needn't handle non-finite values.
Results may differ from the reference program's by a relative error of at most 0.018.
Values may be sent and summed in bfloat16 or wider, within the bound.
A program may use at most 64 MiB of HBM per device.

```python
import math
import jax
import jax.numpy as jnp
from jax import lax

D = 2048
HEADS = 8
DK = 128
DV = 128
CONV_CH = 1024
BLOCK = 64
TOK_DEV = 256
TOKENS = 4096
HEAD_GROUPS = 2


def draw_floor_gap(key, part):
    subkeys = jax.random.split(jax.random.fold_in(key, 11), 3)
    share_fast = 0.5
    fast_heads = jax.random.uniform(subkeys[0], (HEADS, 1), jnp.float32) < share_fast
    fast_gap = jnp.exp(jax.random.uniform(subkeys[1], (HEADS, DK), jnp.float32, math.log(0.02), math.log(0.06)))
    slow_gap = jnp.exp(jax.random.uniform(subkeys[2], (HEADS, DK), jnp.float32, math.log(0.1), math.log(0.5))) / TOKENS
    return jnp.where(fast_heads, fast_gap, slow_gap).astype(jnp.float32)


def draw_extra_decay(key, part):
    subkeys = jax.random.split(jax.random.fold_in(key, 23), 3)
    groups = TOKENS // TOK_DEV
    levels = jnp.exp(jax.random.uniform(subkeys[0], (groups, HEADS), jnp.float32, math.log(0.2), math.log(0.8)))
    filtered_signal = -jnp.repeat(levels, TOK_DEV, axis=0) / TOKENS
    location_indices = jax.random.randint(subkeys[1], (2, HEADS), 0, TOKENS)
    stack_tiers = jax.random.uniform(subkeys[2], (2, HEADS), jnp.float32, 0.22, 0.45)
    location_entries = jnp.arange(TOKENS)[None, :, None]
    segment_clusters = jnp.sum(jnp.where(location_entries == location_indices[:, None, :], -stack_tiers[:, None, :], 0.0), axis=0)
    return (filtered_signal + segment_clusters).astype(jnp.float32)


def steps_of(stream_key, extent, cuts, least, high):
    gain = 1.0
    for dim, blocks in cuts:
        steps = jax.random.uniform(jax.random.fold_in(jax.random.fold_in(stream_key, 6), dim), (blocks,), jnp.float32, least / len(cuts), high / len(cuts))
        gain = gain * jnp.repeat(jnp.exp(steps), extent[dim] // blocks).reshape((-1,) + (1,) * (len(extent) - 1 - dim))
    return gain


def bell_draw(own_key, extent, width, bound, cuts=(), dtype=jnp.bfloat16):
    entries = width * jax.random.normal(own_key, extent, jnp.float32)
    if cuts:
        entries = entries * steps_of(own_key, extent, cuts, -0.22, 0.18)
    return jnp.clip(entries, -bound, bound).astype(dtype)


def setup_inputs(seed: int = 0) -> dict:
    arg_keys = jax.random.split(jax.random.key(seed), 17)
    tokens = bell_draw(arg_keys[0], (TOKENS, D), 1.0, 6.0, ((0, 32),))
    norm_gain = jnp.clip(1.0 + 0.18 * jax.random.normal(arg_keys[1], (D,), jnp.float32), 0.1, 1.9)
    w_query = bell_draw(arg_keys[2], (D, HEADS * DK), D ** -0.5, 0.125, ((0, 16), (1, 2)))
    w_forget = bell_draw(arg_keys[3], (D, HEADS * DK), D ** -0.5, 0.125, ((0, 16), (1, 2)))
    w_input = bell_draw(arg_keys[4], (D, HEADS * DV), D ** -0.5, 0.125, ((0, 16), (1, 2)))
    w_outgate = bell_draw(arg_keys[5], (D, HEADS * DV), D ** -0.5, 0.125, ((0, 16), (1, 2)))
    w_bgate = bell_draw(arg_keys[6], (D, CONV_CH), D ** -0.5, 0.125, ((0, 16), (1, 2)))
    w_cgate = bell_draw(arg_keys[7], (D, CONV_CH), D ** -0.5, 0.125, ((0, 16), (1, 2)))
    w_value = bell_draw(arg_keys[8], (D, CONV_CH), D ** -0.5, 0.125, ((0, 16), (1, 2)))
    floor_gap = draw_floor_gap(jax.random.fold_in(arg_keys[16], 71), 0)
    extra_decay = draw_extra_decay(jax.random.fold_in(arg_keys[16], 71), 0)
    start_state = bell_draw(arg_keys[11], (HEADS, DK, DV), (30.0 / TOKENS), 0.109375, ((0, 2),), jnp.float32)
    state_gain = jnp.clip(1.0 + 0.18 * jax.random.normal(arg_keys[12], (DV,), jnp.float32), 0.1, 1.9)
    conv_taps = bell_draw(arg_keys[13], (3, CONV_CH), 0.6, 3.0, ((1, 2),), jnp.float32)
    out_rec = bell_draw(arg_keys[14], (HEADS * DV, D), (HEADS * DV + CONV_CH) ** -0.5, 0.125, ((0, 2), (1, 16)))
    out_conv = bell_draw(arg_keys[15], (CONV_CH, D), (HEADS * DV + CONV_CH) ** -0.5, 0.125, ((0, 2), (1, 16)))
    return {"tokens": tokens, "norm_gain": norm_gain, "w_query": w_query, "w_forget": w_forget, "w_input": w_input, "w_outgate": w_outgate, "w_bgate": w_bgate, "w_cgate": w_cgate, "w_value": w_value, "floor_gap": floor_gap, "extra_decay": extra_decay, "start_state": start_state, "state_gain": state_gain, "conv_taps": conv_taps, "out_rec": out_rec, "out_conv": out_conv}


eps = 1e-06
highest_precision = lax.Precision.HIGHEST

def rms_scale(values):
    return lax.rsqrt(lax.optimization_barrier(jnp.mean(values * values, axis=-1, keepdims=True)) + eps)

def recurrence(queries, write_in, inputs, log_keep, initial, block_len):
    length, head_count, address_feature_count = queries.shape
    blocks_count = length // block_len

    def blocked(tensor):
        return tensor.reshape(blocks_count, block_len, head_count, tensor.shape[-1]).transpose(0, 2, 1, 3)
    causal = (jnp.arange(block_len)[:, None] >= jnp.arange(block_len)[None, :])[None, :, :, None]

    def advance(memory_state, pieces):
        query_block, write_blk, input_block, keep_blk = pieces
        running_state = jnp.cumsum(keep_blk, axis=1)
        spread = running_state[:, :, None, :] - running_state[:, None, :, :]
        decays = jnp.where(causal, jnp.exp(jnp.minimum(spread, 0.0)), 0.0)
        scores = lax.optimization_barrier(jnp.sum(query_block[:, :, None, :] * write_blk[:, None, :, :] * decays, axis=-1))
        final_output = jnp.einsum('qcp,qpi->qci', query_block * jnp.exp(running_state), memory_state, precision=highest_precision)
        final_output = final_output + jnp.einsum('hts,hsv->htv', scores, input_block, precision=highest_precision)
        final_state = running_state[:, -1, :]
        weighted_value = write_blk * jnp.exp(final_state[:, None, :] - running_state)
        memory_state = memory_state * jnp.exp(final_state)[:, :, None] + jnp.einsum('euz,eul->ezl', weighted_value, input_block, precision=highest_precision)
        return (memory_state, final_output)
    memory_state, output_list = lax.scan(advance, initial, (blocked(queries), blocked(write_in), blocked(inputs), blocked(log_keep)))
    return output_list.transpose(0, 2, 1, 3).reshape(length, head_count, output_list.shape[-1])

def reference(tokens, norm_gain, w_query, w_forget, w_input, w_outgate, w_bgate, w_cgate, w_value, floor_gap, extra_decay, start_state, state_gain, conv_taps, out_rec, out_conv):
    tokens_f = tokens.astype(jnp.float32)
    normed = (tokens_f * rms_scale(tokens_f) * norm_gain).astype(jnp.bfloat16)

    def project(matrix):
        return jnp.dot(normed, matrix, preferred_element_type=jnp.float32).astype(jnp.bfloat16)
    query_raw = project(w_query)
    forget_raw = project(w_forget)
    input_raw = project(w_input)
    outgate_raw = project(w_outgate)
    bgate_raw = project(w_bgate)
    cgate_raw = project(w_cgate)
    value_raw = project(w_value)
    length = normed.shape[0]
    queries = jax.nn.silu(query_raw.astype(jnp.float32)).reshape(length, HEADS, DK)
    write_in = floor_gap[None] * jax.nn.sigmoid(-forget_raw.astype(jnp.float32)).reshape(length, HEADS, DK)
    log_keep = jnp.log1p(-write_in) + extra_decay[:, :, None]
    inputs = input_raw.astype(jnp.float32).reshape(length, HEADS, DV)
    blended_state = recurrence(queries, write_in, inputs, log_keep, start_state, BLOCK)
    gate_out = jax.nn.silu(outgate_raw.astype(jnp.float32)).reshape(length, HEADS, DV)
    rec_out = (blended_state * rms_scale(blended_state) * state_gain * gate_out).reshape(length, HEADS * DV).astype(jnp.bfloat16)
    gated = cgate_raw.astype(jnp.float32) * value_raw.astype(jnp.float32)
    padded = jnp.concatenate([jnp.zeros((2, gated.shape[1]), jnp.float32), gated], axis=0)
    conv_out = conv_taps[0] * padded[:length] + conv_taps[1] * padded[1:length + 1] + conv_taps[2] * padded[2:]
    short_out = (bgate_raw.astype(jnp.float32) * conv_out).astype(jnp.bfloat16)
    rec_width = HEADS * DV // HEAD_GROUPS
    conv_width = CONV_CH // HEAD_GROUPS
    mixed_sum = jnp.zeros((length, out_rec.shape[1]), jnp.float32)
    for group in range(HEAD_GROUPS):
        rec_lo = group * rec_width
        conv_lo = group * conv_width
        partial_value = jnp.dot(rec_out[:, rec_lo:rec_lo + rec_width], out_rec[rec_lo:rec_lo + rec_width], preferred_element_type=jnp.float32)
        partial_value = partial_value + jnp.dot(short_out[:, conv_lo:conv_lo + conv_width], out_conv[conv_lo:conv_lo + conv_width], preferred_element_type=jnp.float32)
        rounded = lax.optimization_barrier(partial_value.astype(jnp.bfloat16))
        mixed_sum = mixed_sum + rounded.astype(jnp.float32)
    return mixed_sum.astype(jnp.bfloat16)
```

```python
import functools

import jax
import jax.numpy as jnp
from jax import lax
from jax.experimental import pallas as pl
from jax.experimental.pallas import tpu as pltpu
from jax.sharding import PartitionSpec as P

BLOCK = 64


eps = 1e-06
highest_precision = lax.Precision.HIGHEST


def prefix(value, axis, join, neutral):
    count, mine = (lax.axis_size(axis), lax.axis_index(axis))
    pieces = jax.tree.map(lambda part: lax.all_gather(part, axis), value)
    so_far = jax.tree.map(
        lambda part, zero: jnp.full_like(part, 0) + jnp.asarray(zero, part.dtype), value, neutral
    )

    def hop(position, so_far):
        longer = join(so_far, jax.tree.map(lambda part: part[position], pieces))
        return jax.tree.map(lambda new, old: jnp.where(position < mine, new, old), longer, so_far)

    return lax.fori_loop(0, count - 1, hop, so_far)


def shifted(block, axis, distance):
    devices = range(lax.axis_size(axis))
    route = [(i - distance, i) for i in devices if i - distance in devices]
    return lax.ppermute(block, axis, route)


def rms_scale(values):
    return lax.rsqrt(jnp.mean(values * values, axis=-1, keepdims=True) + eps)


def local_blocks(queries, write_in, inputs, log_keep, block_len):
    length, head_count, address_feature_count = queries.shape
    value_dim = inputs.shape[-1]
    blocks_count = length // block_len

    def blocked(tensor):
        return tensor.reshape(blocks_count, block_len, head_count, tensor.shape[-1]).transpose(
            0, 2, 1, 3
        )

    def unblock(tensor):
        return tensor.transpose(0, 2, 1, 3).reshape(length, head_count, tensor.shape[-1])

    causal = (jnp.arange(block_len)[:, None] >= jnp.arange(block_len)[None, :])[None, :, :, None]

    def advance(carried, pieces):
        memory_state, offset = carried
        query_block, write_blk, input_block, keep_blk = pieces
        running_state = jnp.cumsum(keep_blk, axis=1)
        spread = running_state[:, :, None, :] - running_state[:, None, :, :]
        decays = jnp.where(causal, jnp.exp(jnp.minimum(spread, 0.0)), 0.0)
        scores = jnp.sum(query_block[:, :, None, :] * write_blk[:, None, :, :] * decays, axis=-1)
        final_output = jnp.einsum(
            "qcp,qpi->qci",
            query_block * jnp.exp(running_state),
            memory_state,
            precision=highest_precision,
        )
        final_output = final_output + jnp.einsum(
            "hts,hsv->htv", scores, input_block, precision=highest_precision
        )
        lifted_state = query_block * jnp.exp(running_state + offset[:, None, :])
        final_state = running_state[:, -1, :]
        weighted_value = write_blk * jnp.exp(final_state[:, None, :] - running_state)
        memory_state = memory_state * jnp.exp(final_state)[:, :, None] + jnp.einsum(
            "euz,eul->ezl", weighted_value, input_block, precision=highest_precision
        )
        return ((memory_state, offset + final_state), (final_output, lifted_state))

    initial = (
        jnp.zeros((head_count, address_feature_count, value_dim), jnp.float32),
        jnp.zeros((head_count, address_feature_count), jnp.float32),
    )
    finals, outputs = lax.scan(
        advance, initial, (blocked(queries), blocked(write_in), blocked(inputs), blocked(log_keep))
    )
    return (unblock(outputs[0]), unblock(outputs[1]), finals[0], jnp.exp(finals[1]))


def chain(earlier, later):
    return (earlier[0] * later[0], earlier[1] * later[0][:, :, None] + later[1])


def on_device(
    tokens,
    norm_gain,
    w_query,
    w_forget,
    w_input,
    w_outgate,
    w_bgate,
    w_cgate,
    w_value,
    floor_gap,
    extra_decay,
    start_state,
    state_gain,
    conv_taps,
    out_rec,
    out_conv,
):
    tokens_f = tokens.astype(jnp.float32)
    normed = (tokens_f * rms_scale(tokens_f) * norm_gain).astype(jnp.bfloat16)
    weights = (w_query, w_forget, w_input, w_outgate, w_bgate, w_cgate, w_value)
    whole_weights = (
        lax.all_gather(w_query, "sp", axis=0, tiled=True),
        lax.all_gather(w_forget, "sp", axis=0, tiled=True),
        lax.all_gather(w_input, "sp", axis=0, tiled=True),
        lax.all_gather(w_outgate, "sp", axis=0, tiled=True),
        lax.all_gather(w_bgate, "sp", axis=0, tiled=True),
        lax.all_gather(w_cgate, "sp", axis=0, tiled=True),
        lax.all_gather(w_value, "sp", axis=0, tiled=True),
    )

    def project(shard_rows):
        return jnp.concatenate(
            [
                jnp.dot(shard_rows, matrix, preferred_element_type=jnp.float32).astype(jnp.bfloat16)
                for matrix in whole_weights
            ],
            axis=1,
        )

    joined = project(lax.all_gather(normed, "tp", axis=0, tiled=True))
    borders = [0]
    for matrix in weights:
        borders.append(borders[-1] + matrix.shape[1])
    projected = [joined[:, borders[number] : borders[number + 1]] for number in range(len(weights))]
    query_raw, forget_raw, input_raw, outgate_raw, bgate_raw, cgate_raw, value_raw = projected
    length = query_raw.shape[0]
    head_count, address_feature_count = floor_gap.shape
    value_dim = start_state.shape[2]
    queries = jax.nn.silu(query_raw.astype(jnp.float32)).reshape(
        length, head_count, address_feature_count
    )
    write_in = floor_gap[None] * jax.nn.sigmoid(-forget_raw.astype(jnp.float32)).reshape(
        length, head_count, address_feature_count
    )
    log_keep = jnp.log1p(-write_in) + extra_decay[:, :, None]
    inputs = input_raw.astype(jnp.float32).reshape(length, head_count, value_dim)
    output_list, lifted_state, memory_state, kept = local_blocks(
        queries, write_in, inputs, log_keep, BLOCK
    )
    before_keep, before_memory = prefix(
        (kept, memory_state), "sp", chain, (jnp.ones_like(kept), jnp.zeros_like(memory_state))
    )
    carried_hidden_prior = start_state * before_keep[:, :, None] + before_memory
    blended_state = output_list + jnp.einsum(
        "sqa,qar->sqr", lifted_state, carried_hidden_prior, precision=highest_precision
    )
    gate_out = jax.nn.silu(outgate_raw.astype(jnp.float32)).reshape(length, head_count, value_dim)
    rec_out = (
        (blended_state * rms_scale(blended_state) * state_gain * gate_out)
        .reshape(length, head_count * value_dim)
        .astype(jnp.bfloat16)
    )
    rim_rows = jnp.stack([cgate_raw[length - 2 :], value_raw[length - 2 :]])
    before_rim = shifted(rim_rows, "sp", 1)
    convolution_gate_widened = jnp.concatenate([before_rim[0], cgate_raw], axis=0).astype(
        jnp.float32
    )
    value_ext = jnp.concatenate([before_rim[1], value_raw], axis=0).astype(jnp.float32)
    gated = convolution_gate_widened * value_ext
    conv_out = (
        conv_taps[0] * gated[:length]
        + conv_taps[1] * gated[1 : length + 1]
        + conv_taps[2] * gated[2:]
    )
    short_out = (bgate_raw.astype(jnp.float32) * conv_out).astype(jnp.bfloat16)
    rec_weight, conv_weight = (
        lax.all_gather(out_rec, "sp", axis=1, tiled=True),
        lax.all_gather(out_conv, "sp", axis=1, tiled=True),
    )
    product = jnp.dot(rec_out, rec_weight, preferred_element_type=jnp.float32)
    return lax.psum_scatter(
        (product + jnp.dot(short_out, conv_weight, preferred_element_type=jnp.float32)).astype(
            jnp.bfloat16
        ),
        "tp",
        scatter_dimension=0,
        tiled=True,
    )


MESH = pl.DeviceIdType.MESH
f32, bf16 = jnp.float32, jnp.bfloat16


def high_dot(a, b, dims):
    return lax.dot_general(
        a, b, (dims, ((), ())), precision=highest_precision, preferred_element_type=f32
    )


def sigmoid(v):
    return 1.0 / (1.0 + jnp.exp(-v))


def fused_kernel(
    heads,
    lines,
    groups,
    block,
    tok_ref,
    gain_ref,
    w_ref,
    o_ref,
    gap_ref,
    ed_ref,
    start_ref,
    sgain_ref,
    taps_ref,
    out_ref,
    tg,
    gw,
    go,
    ge,
    proj,
    gated,
    mixed,
    lifted,
    lhs,
    packet,
    packets,
    state,
    part,
    r0,
    r1a,
    r1b,
    r2,
    s_w,
    s_o,
    s_e,
    s_t,
    s_p,
    sr_w,
    sl_w,
    sr_o,
    sl_o,
    v_w,
    v_o,
    v_e,
    v_t,
    v_p,
    s_x0,
    v_x0,
    s_x1,
    v_x1,
    s_x2,
    v_x2,
):
    s_me, t_me = lax.axis_index("sp"), lax.axis_index("tp")
    q, r = s_me // heads, lax.rem(s_me, heads)
    e_me = r * groups + t_me
    every = heads * groups
    rows = tok_ref.shape[0]
    key = w_ref.shape[2] // 7
    length = every * rows

    def copy(src, dst, send, recv, dev):
        return pltpu.make_async_remote_copy(
            src_ref=src, dst_ref=dst, send_sem=send, recv_sem=recv, device_id=dev,
            device_id_type=MESH,
        )

    def in_group(e):
        return (q * heads + e // groups, lax.rem(e, groups))

    def along(p):
        return (p * heads + r, t_me)

    barrier = pltpu.get_barrier_semaphore()
    for d in range(1, every):
        pl.semaphore_signal(
            barrier, inc=1, device_id=in_group(lax.rem(e_me + d, every)), device_id_type=MESH
        )
    for d in range(1, lines):
        pl.semaphore_signal(
            barrier, inc=1, device_id=along(lax.rem(q + d, lines)), device_id_type=MESH
        )
    pl.semaphore_wait(barrier, every - 1 + lines - 1)

    has_right, has_left = q + 1 < lines, q > 0
    right = along(lax.rem(q + 1, lines))
    left = along(lax.rem(q + lines - 1, lines))

    def moves(src, dst, send_r, send_l, recv, s):
        return (
            copy(src, dst.at[s], send_r.at[s], recv.at[s], right),
            copy(src, dst.at[s], send_l.at[s], recv.at[s], left),
        )

    def forward(src, dst, send_r, send_l, recv, s, to_right=True, to_left=True):
        go_right, go_left = moves(src, dst, send_r, send_l, recv, s)
        if to_right:
            pl.when(has_right)(go_right.start)
        if to_left:
            pl.when(has_left)(go_left.start)

    W = (gw, sr_w, sl_w, v_w)
    O = (go, sr_o, sl_o, v_o)

    def swaps(ref, dst, send, recv):
        found = []
        for j in range(1, heads):
            other = lax.rem(r + j, heads)
            found.append(
                copy(ref.at[other], dst, send.at[j], recv, (q * heads + other, t_me))
            )
        return found

    w_swaps = swaps(w_ref, gw.at[s_me], s_w, v_w.at[s_me])
    e_swaps = swaps(ed_ref, ge.at[r], s_e, v_e.at[r])
    o_swaps = swaps(o_ref, go.at[s_me], s_o, v_o.at[s_me])
    t_sends = []
    for d in range(1, every):
        t_sends.append(
            copy(tok_ref, tg.at[e_me], s_t.at[d], v_t.at[e_me], in_group(lax.rem(e_me + d, every)))
        )
    for c in w_swaps:
        c.start()
    forward(w_ref.at[r], *W, s_me)
    for c in e_swaps + o_swaps + t_sends:
        c.start()
    gw[s_me] = w_ref[r]
    go[s_me] = o_ref[r]
    ge[r] = ed_ref[r]
    tg[e_me] = tok_ref[...]

    def arrived(dst, recv, s):
        copy(dst.at[s], dst.at[s], s_p.at[0], recv.at[s], right).wait_recv()

    def relay_own(kind):
        for j in range(1, heads):
            s = q * heads + lax.rem(r + j, heads)
            arrived(kind[0], kind[3], s)
            forward(kind[0].at[s], *kind, s)

    def relay(kind, k):
        for j in range(heads):
            rr = lax.rem(r + j, heads)

            @pl.when(q >= k)
            def _():
                s = (q - k) * heads + rr
                arrived(kind[0], kind[3], s)
                forward(kind[0].at[s], *kind, s, to_left=False)

            @pl.when(q + k < lines)
            def _():
                s = (q + k) * heads + rr
                arrived(kind[0], kind[3], s)
                forward(kind[0].at[s], *kind, s, to_right=False)

    relay_own(W)
    for k in range(1, lines):
        relay(W, k)
        if k == lines - 2:
            forward(o_ref.at[r], *O, s_me)
            relay_own(O)

    for d in range(1, every):
        arrived(tg, v_t, lax.rem(e_me + d, every))

    step = 16

    def norm(i, _):
        e = i // (rows // step)
        at = pl.ds(pl.multiple_of(lax.rem(i, rows // step) * step, step), step)
        x = tg[e, at, :].astype(f32)
        tg[e, at, :] = (x * rms_scale(x) * gain_ref[...]).astype(bf16)
        return 0

    lax.fori_loop(0, length // step, norm, 0)

    depth = heads * w_ref.shape[1]
    tall = 2 * rows

    def project(i, _):
        at = pl.ds(pl.multiple_of(i * tall, tall), tall)
        acc = jnp.zeros((tall, 7 * key), f32)
        for p in range(lines):
            x = tg[pl.ds(i * 2, 2), :, pl.ds(p * depth, depth)].reshape(tall, depth)
            w = gw[pl.ds(p * heads, heads)].reshape(depth, 7 * key)
            acc = acc + jnp.dot(x, w, preferred_element_type=f32)
        proj[at, :] = acc.astype(bf16)
        return 0

    lax.fori_loop(0, length // tall, project, 0)
    for k in range(1, lines - 1):
        relay(O, k)
    for j in range(1, heads):
        arrived(ge, v_e, lax.rem(r + j, heads))

    def column(at, number):
        return proj[at, number * key : (number + 1) * key].astype(f32)

    pad = 8
    blocks = length // block
    per = blocks // heads
    tri = (
        lax.broadcasted_iota(jnp.int32, (block, block), 0)
        >= lax.broadcasted_iota(jnp.int32, (block, block), 1)
    ).astype(f32)
    wide = (
        lax.broadcasted_iota(jnp.int32, (block, key), 0)
        >= lax.broadcasted_iota(jnp.int32, (block, key), 1)
    ).astype(f32)
    gap = gap_ref[pl.ds(r, 1), :]
    packet[...] = jnp.zeros_like(packet)

    def advance(b, _):
        at = pl.ds(pl.multiple_of(b * block, block), block)
        query = column(at, 0)
        query = query * sigmoid(query)
        write = gap * sigmoid(-column(at, 1))
        values = column(at, 2)
        extra = ge[b // per, pl.ds(lax.rem(b, per), 1), :]
        run = high_dot(tri, jnp.log1p(-write), ((1,), (0,))) + jnp.sum(
            wide * extra, axis=1, keepdims=True
        )
        final = run[block - 1 : block, :]
        middle = 0.5 * final
        scores = tri * high_dot(
            query * jnp.exp(run - middle), write * jnp.exp(middle - run), ((1,), (1,))
        )
        before = packet[:key, :]
        offset = packet[key : key + 1, :]
        lift = query * jnp.exp(run)
        mixed[at, :] = high_dot(scores, values, ((1,), (0,))) + high_dot(
            lift, before, ((1,), (1,))
        )
        lifted[at, :] = lift * jnp.exp(offset)
        packet[:key, :] = before * jnp.exp(final) + high_dot(
            values, write * jnp.exp(final - run), ((0,), (0,))
        )
        packet[key : key + pad, :] = jnp.broadcast_to(offset + final, (pad, key))
        gated[pl.ds(pl.multiple_of(b * block + pad, pad), block), :] = column(at, 5) * column(at, 6)
        return 0

    lax.fori_loop(0, blocks, advance, 0)
    packet[key + pad : key + 2 * pad, :] = gated[length : length + pad, :]

    def packet_to(d):
        return copy(
            packet, packets.at[q], s_p.at[d], v_p.at[q], along(lax.rem(q + d, lines))
        )

    for d in range(1, lines):
        pl.when(q + d < lines)(packet_to(d).start)
    state[...] = start_ref[r].T
    gated[:pad, :] = jnp.zeros((pad, key), f32)
    relay(O, lines - 1)
    for p in range(lines - 1):

        @pl.when(p < q)
        def _():
            arrived(packets, v_p, p)
            state[...] = state[...] * jnp.exp(packets[p, key : key + 1, :]) + packets[p, :key, :]

        @pl.when(p + 1 == q)
        def _():
            gated[:pad, :] = packets[p, key + pad : key + 2 * pad, :]

    taps = taps_ref[r]
    for i in range(every):
        lo = i * rows
        at = pl.ds(lo, rows)
        m = mixed[at, :] + high_dot(lifted[at, :], state[...], ((1,), (1,)))
        gate = column(at, 3)
        rec = m * rms_scale(m) * sgain_ref[...] * (gate * sigmoid(gate))
        conv = (
            taps[0:1] * gated[lo + pad - 2 : lo + pad - 2 + rows, :]
            + taps[1:2] * gated[lo + pad - 1 : lo + pad - 1 + rows, :]
            + taps[2:3] * gated[lo + pad : lo + pad + rows, :]
        )
        lhs[at, :key] = rec.astype(bf16)
        lhs[at, key:] = (column(at, 4) * conv).astype(bf16)

    span = o_ref.shape[2]
    width = span * heads * lines
    half = width // 2

    def expand(i, _):
        for p in range(heads * lines // 2):
            w = jnp.concatenate([go[2 * p], go[2 * p + 1]], axis=1)
            part[i, :, 2 * span * p : 2 * span * (p + 1)] = jnp.dot(
                lhs[pl.ds(pl.multiple_of(i * rows, rows), rows), :], w, preferred_element_type=f32
            ).astype(bf16)
        return 0

    lax.fori_loop(0, every, expand, 0)

    y, c = r // 2, lax.rem(r, 2)
    cc, yy, xx = 1 - c, 1 - y, 1 - t_me

    def slot(y, c, x):
        return (y * 2 + c) * groups + x

    core = (q * heads + y * 2 + cc, t_me)
    over_y = (q * heads + yy * 2 + c, t_me)
    over_x = (s_me, xx)
    lo, hi = pl.ds(0, half), pl.ds(half, half)
    first = []
    for a in range(2):
        for b in range(2):
            n = 2 * a + b
            first.append(copy(part.at[slot(a, cc, b)], r0.at[n], s_x0.at[n], v_x0.at[n], core))
    for d in first:
        d.start()

    def add(e, cols, other):
        return part[e, :, cols].astype(f32) + other.astype(f32)

    for d in first:
        d.wait()
    for a in range(2):
        for b in range(2):
            e = slot(a, c, b)
            part[e] = (part[e].astype(f32) + r0[2 * a + b].astype(f32)).astype(bf16)
    second = []
    for b in range(2):
        second.append(
            copy(part.at[slot(yy, c, b), :, lo], r1a.at[b], s_x1.at[b], v_x1.at[b], over_y)
        )
        second.append(
            copy(part.at[slot(b, c, xx), :, hi], r1b.at[b], s_x1.at[2 + b], v_x1.at[2 + b], over_x)
        )
    for d in second:
        d.start()
    for d in second:
        d.wait()
    part[slot(y, c, xx), :, lo] = add(slot(y, c, xx), lo, r1a[xx]).astype(bf16)
    part[slot(yy, c, t_me), :, hi] = add(slot(yy, c, t_me), hi, r1b[yy]).astype(bf16)
    third = [
        copy(part.at[slot(y, c, xx), :, lo], r2.at[0], s_x2.at[0], v_x2.at[0], over_x),
        copy(part.at[slot(yy, c, t_me), :, hi], r2.at[1], s_x2.at[1], v_x2.at[1], over_y),
    ]
    for d in third:
        d.start()
    mine = slot(y, c, t_me)
    for d in third:
        d.wait()
    out_ref[:, lo] = (add(mine, lo, r1a[t_me]) + r2[0].astype(f32)).astype(bf16)
    out_ref[:, hi] = (add(mine, hi, r1b[y]) + r2[1].astype(f32)).astype(bf16)

    for c in w_swaps + e_swaps + o_swaps + t_sends:
        c.wait_send()
    for d in range(1, lines):
        pl.when(q + d < lines)(packet_to(d).wait_send)

    for kind in (W, O):
        for p in range(lines):
            for j in range(heads):
                s = p * heads + j
                go_right, go_left = moves(kind[0].at[s], *kind, s)
                pl.when(jnp.logical_and(has_right, p <= q))(go_right.wait_send)
                pl.when(jnp.logical_and(has_left, p >= q))(go_left.wait_send)


def fused(heads, lines, groups, *args):
    (tokens, norm_gain, w_query, w_forget, w_input, w_outgate, w_bgate, w_cgate, w_value,
     floor_gap, extra_decay, start_state, state_gain, conv_taps, out_rec, out_conv) = args
    rows, model = tokens.shape
    depth = w_query.shape[0]
    key = floor_gap.shape[1]
    span = out_rec.shape[1]
    every = heads * groups
    length = every * rows
    sp = heads * lines
    pad = 8

    def by_head(tensor):
        return tensor.reshape(tensor.shape[0], heads, key).transpose(1, 0, 2)

    weights = jnp.concatenate(
        [by_head(w) for w in (w_query, w_forget, w_input, w_outgate, w_bgate, w_cgate, w_value)],
        axis=2,
    )
    outs = jnp.concatenate(
        [out_rec.reshape(heads, key, span), out_conv.reshape(heads, key, span)], axis=1
    )
    per = extra_decay.shape[0] // BLOCK
    extra = extra_decay.T.reshape(heads, per, BLOCK)
    extra = jnp.pad(extra, ((0, 0), (0, pad - per), (0, key - BLOCK)))
    taps = jnp.pad(by_head(conv_taps), ((0, 0), (0, pad - conv_taps.shape[0]), (0, 0)))
    dma = pltpu.SemaphoreType.DMA
    half = model // 2
    scratch = [
        pltpu.VMEM((every, rows, model), bf16),
        pltpu.VMEM((sp, depth, 7 * key), bf16),
        pltpu.VMEM((sp, 2 * key, span), bf16),
        pltpu.VMEM((heads, pad, key), f32),
        pltpu.VMEM((length, 7 * key), bf16),
        pltpu.VMEM((length + pad, key), f32),
        pltpu.VMEM((length, key), f32),
        pltpu.VMEM((length, key), f32),
        pltpu.VMEM((length, 2 * key), bf16),
        pltpu.VMEM((key + 2 * pad, key), f32),
        pltpu.VMEM((lines, key + 2 * pad, key), f32),
        pltpu.VMEM((key, key), f32),
        pltpu.VMEM((every, rows, model), bf16),
        pltpu.VMEM((every // 2, rows, model), bf16),
        pltpu.VMEM((2, rows, half), bf16),
        pltpu.VMEM((2, rows, half), bf16),
        pltpu.VMEM((2, rows, half), bf16),
        dma((heads,)), dma((heads,)), dma((heads,)), dma((every,)), dma((lines,)),
        dma((sp,)), dma((sp,)), dma((sp,)), dma((sp,)),
        dma((sp,)), dma((sp,)), dma((heads,)), dma((every,)), dma((lines,)),
        dma((4,)), dma((4,)), dma((4,)), dma((4,)), dma((2,)), dma((2,)),
    ]
    return pl.pallas_call(
        functools.partial(fused_kernel, heads, lines, groups, BLOCK),
        out_shape=jax.ShapeDtypeStruct((rows, model), bf16),
        in_specs=[pl.BlockSpec(memory_space=pltpu.VMEM)] * 9,
        out_specs=pl.BlockSpec(memory_space=pltpu.VMEM),
        scratch_shapes=scratch,
        compiler_params=pltpu.CompilerParams(
            collective_id=0, has_side_effects=True, vmem_limit_bytes=60 * 1024 * 1024
        ),
        name="mixer",
    )(tokens, norm_gain[None], weights, outs, floor_gap, extra, start_state, state_gain[None], taps)


def per_device(sp, tp, *args):
    heads = args[9].shape[0]
    fits = (
        heads == 4 and tp == 2 and sp % heads == 0
        and args[14].shape[1] % 128 == 0
        and args[13].shape[1] == heads * args[9].shape[1]
        and args[10].shape[0] % BLOCK == 0
    )
    if not fits:
        return on_device(*args)
    return fused(heads, sp // heads, tp, *args)


def solution(mesh):
    placed = (
        P(("sp", "tp"), None),
        P(),
        P("sp", "tp"),
        P("sp", "tp"),
        P("sp", "tp"),
        P("sp", "tp"),
        P("sp", "tp"),
        P("sp", "tp"),
        P("sp", "tp"),
        P("tp", None),
        P("sp", "tp"),
        P("tp", None, None),
        P(),
        P(None, "tp"),
        P("tp", "sp"),
        P("tp", "sp"),
    )
    return jax.shard_map(
        functools.partial(per_device, mesh.shape["sp"], mesh.shape["tp"]), mesh=mesh, in_specs=placed, out_specs=P(("sp", "tp"), None), check_vma=False
    )
```

```python
import functools

import jax
import jax.numpy as jnp
from jax import lax
from jax.experimental import pallas as pl
from jax.experimental.pallas import tpu as pltpu
from jax.sharding import PartitionSpec as P

BLOCK = 64


eps = 1e-06
highest_precision = lax.Precision.HIGHEST


def prefix(value, axis, join, neutral):
    count, mine = (lax.axis_size(axis), lax.axis_index(axis))
    pieces = jax.tree.map(lambda part: lax.all_gather(part, axis), value)
    so_far = jax.tree.map(
        lambda part, zero: jnp.full_like(part, 0) + jnp.asarray(zero, part.dtype), value, neutral
    )

    def hop(position, so_far):
        longer = join(so_far, jax.tree.map(lambda part: part[position], pieces))
        return jax.tree.map(lambda new, old: jnp.where(position < mine, new, old), longer, so_far)

    return lax.fori_loop(0, count - 1, hop, so_far)


def shifted(block, axis, distance):
    devices = range(lax.axis_size(axis))
    route = [(i - distance, i) for i in devices if i - distance in devices]
    return lax.ppermute(block, axis, route)


def rms_scale(values):
    return lax.rsqrt(jnp.mean(values * values, axis=-1, keepdims=True) + eps)


def local_blocks(queries, write_in, inputs, log_keep, block_len):
    length, head_count, address_feature_count = queries.shape
    value_dim = inputs.shape[-1]
    blocks_count = length // block_len

    def blocked(tensor):
        return tensor.reshape(blocks_count, block_len, head_count, tensor.shape[-1]).transpose(
            0, 2, 1, 3
        )

    def unblock(tensor):
        return tensor.transpose(0, 2, 1, 3).reshape(length, head_count, tensor.shape[-1])

    causal = (jnp.arange(block_len)[:, None] >= jnp.arange(block_len)[None, :])[None, :, :, None]

    def advance(carried, pieces):
        memory_state, offset = carried
        query_block, write_blk, input_block, keep_blk = pieces
        running_state = jnp.cumsum(keep_blk, axis=1)
        spread = running_state[:, :, None, :] - running_state[:, None, :, :]
        decays = jnp.where(causal, jnp.exp(jnp.minimum(spread, 0.0)), 0.0)
        scores = jnp.sum(query_block[:, :, None, :] * write_blk[:, None, :, :] * decays, axis=-1)
        final_output = jnp.einsum(
            "qcp,qpi->qci",
            query_block * jnp.exp(running_state),
            memory_state,
            precision=highest_precision,
        )
        final_output = final_output + jnp.einsum(
            "hts,hsv->htv", scores, input_block, precision=highest_precision
        )
        lifted_state = query_block * jnp.exp(running_state + offset[:, None, :])
        final_state = running_state[:, -1, :]
        weighted_value = write_blk * jnp.exp(final_state[:, None, :] - running_state)
        memory_state = memory_state * jnp.exp(final_state)[:, :, None] + jnp.einsum(
            "euz,eul->ezl", weighted_value, input_block, precision=highest_precision
        )
        return ((memory_state, offset + final_state), (final_output, lifted_state))

    initial = (
        jnp.zeros((head_count, address_feature_count, value_dim), jnp.float32),
        jnp.zeros((head_count, address_feature_count), jnp.float32),
    )
    finals, outputs = lax.scan(
        advance, initial, (blocked(queries), blocked(write_in), blocked(inputs), blocked(log_keep))
    )
    return (unblock(outputs[0]), unblock(outputs[1]), finals[0], jnp.exp(finals[1]))


def chain(earlier, later):
    return (earlier[0] * later[0], earlier[1] * later[0][:, :, None] + later[1])


def on_device(
    tokens,
    norm_gain,
    w_query,
    w_forget,
    w_input,
    w_outgate,
    w_bgate,
    w_cgate,
    w_value,
    floor_gap,
    extra_decay,
    start_state,
    state_gain,
    conv_taps,
    out_rec,
    out_conv,
):
    tokens_f = tokens.astype(jnp.float32)
    normed = (tokens_f * rms_scale(tokens_f) * norm_gain).astype(jnp.bfloat16)
    weights = (w_query, w_forget, w_input, w_outgate, w_bgate, w_cgate, w_value)
    whole_weights = (
        lax.all_gather(w_query, "sp", axis=0, tiled=True),
        lax.all_gather(w_forget, "sp", axis=0, tiled=True),
        lax.all_gather(w_input, "sp", axis=0, tiled=True),
        lax.all_gather(w_outgate, "sp", axis=0, tiled=True),
        lax.all_gather(w_bgate, "sp", axis=0, tiled=True),
        lax.all_gather(w_cgate, "sp", axis=0, tiled=True),
        lax.all_gather(w_value, "sp", axis=0, tiled=True),
    )

    def project(shard_rows):
        return jnp.concatenate(
            [
                jnp.dot(shard_rows, matrix, preferred_element_type=jnp.float32).astype(jnp.bfloat16)
                for matrix in whole_weights
            ],
            axis=1,
        )

    joined = project(lax.all_gather(normed, "tp", axis=0, tiled=True))
    borders = [0]
    for matrix in weights:
        borders.append(borders[-1] + matrix.shape[1])
    projected = [joined[:, borders[number] : borders[number + 1]] for number in range(len(weights))]
    query_raw, forget_raw, input_raw, outgate_raw, bgate_raw, cgate_raw, value_raw = projected
    length = query_raw.shape[0]
    head_count, address_feature_count = floor_gap.shape
    value_dim = start_state.shape[2]
    queries = jax.nn.silu(query_raw.astype(jnp.float32)).reshape(
        length, head_count, address_feature_count
    )
    write_in = floor_gap[None] * jax.nn.sigmoid(-forget_raw.astype(jnp.float32)).reshape(
        length, head_count, address_feature_count
    )
    log_keep = jnp.log1p(-write_in) + extra_decay[:, :, None]
    inputs = input_raw.astype(jnp.float32).reshape(length, head_count, value_dim)
    output_list, lifted_state, memory_state, kept = local_blocks(
        queries, write_in, inputs, log_keep, BLOCK
    )
    before_keep, before_memory = prefix(
        (kept, memory_state), "sp", chain, (jnp.ones_like(kept), jnp.zeros_like(memory_state))
    )
    carried_hidden_prior = start_state * before_keep[:, :, None] + before_memory
    blended_state = output_list + jnp.einsum(
        "sqa,qar->sqr", lifted_state, carried_hidden_prior, precision=highest_precision
    )
    gate_out = jax.nn.silu(outgate_raw.astype(jnp.float32)).reshape(length, head_count, value_dim)
    rec_out = (
        (blended_state * rms_scale(blended_state) * state_gain * gate_out)
        .reshape(length, head_count * value_dim)
        .astype(jnp.bfloat16)
    )
    rim_rows = jnp.stack([cgate_raw[length - 2 :], value_raw[length - 2 :]])
    before_rim = shifted(rim_rows, "sp", 1)
    convolution_gate_widened = jnp.concatenate([before_rim[0], cgate_raw], axis=0).astype(
        jnp.float32
    )
    value_ext = jnp.concatenate([before_rim[1], value_raw], axis=0).astype(jnp.float32)
    gated = convolution_gate_widened * value_ext
    conv_out = (
        conv_taps[0] * gated[:length]
        + conv_taps[1] * gated[1 : length + 1]
        + conv_taps[2] * gated[2:]
    )
    short_out = (bgate_raw.astype(jnp.float32) * conv_out).astype(jnp.bfloat16)
    rec_weight, conv_weight = (
        lax.all_gather(out_rec, "sp", axis=1, tiled=True),
        lax.all_gather(out_conv, "sp", axis=1, tiled=True),
    )
    product = jnp.dot(rec_out, rec_weight, preferred_element_type=jnp.float32)
    return lax.psum_scatter(
        (product + jnp.dot(short_out, conv_weight, preferred_element_type=jnp.float32)).astype(
            jnp.bfloat16
        ),
        "tp",
        scatter_dimension=0,
        tiled=True,
    )


MESH = pl.DeviceIdType.MESH
f32, bf16 = jnp.float32, jnp.bfloat16


def high_dot(a, b, dims):
    return lax.dot_general(
        a, b, (dims, ((), ())), precision=highest_precision, preferred_element_type=f32
    )


def sigmoid(v):
    return 1.0 / (1.0 + jnp.exp(-v))


def fused_kernel(
    heads,
    lines,
    groups,
    block,
    tok_in,
    gain_ref,
    w_ins,
    rec_in,
    conv_in,
    gap_ref,
    ed_ref,
    start_ref,
    sgain_ref,
    taps_ref,
    out_ref,
    tok_ref,
    w_ref,
    o_ref,
    normed,
    tg,
    gw,
    go,
    ge,
    proj,
    gated,
    mixed,
    lifted,
    packet,
    packets,
    state,
    part,
    r0,
    r1a,
    r1b,
    r2,
    s_w,
    s_o,
    s_e,
    s_t,
    s_p,
    sr_w,
    sl_w,
    sr_o,
    sl_o,
    v_w,
    v_o,
    v_e,
    v_t,
    v_p,
    s_x0,
    v_x0,
    s_x1,
    v_x1,
    s_x2,
    v_x2,
    d_w,
    d_o,
):
    s_me, t_me = lax.axis_index("sp"), lax.axis_index("tp")
    q, r = s_me // heads, lax.rem(s_me, heads)
    e_me = r * groups + t_me
    every = heads * groups
    rows = tok_ref.shape[0]
    key = w_ref.shape[2] // 7
    length = every * rows

    def copy(src, dst, send, recv, dev):
        return pltpu.make_async_remote_copy(
            src_ref=src, dst_ref=dst, send_sem=send, recv_sem=recv, device_id=dev,
            device_id_type=MESH,
        )

    def in_group(e):
        return (q * heads + e // groups, lax.rem(e, groups))

    def along(p):
        return (p * heads + r, t_me)

    staged = []
    for j in range(heads):
        h = lax.rem(r + j, heads)
        for number, w_in in enumerate(w_ins):
            staged.append(
                pltpu.make_async_copy(
                    w_in.at[:, pl.ds(pl.multiple_of(h * key, key), key)],
                    w_ref.at[h, :, number * key : (number + 1) * key],
                    d_w.at[h],
                )
            )
    staged.append(pltpu.make_async_copy(tok_in, tok_ref, d_o.at[0]))
    for h in range(heads):
        at = pl.ds(h * key, key)
        staged.append(pltpu.make_async_copy(rec_in.at[at], o_ref.at[h, :key], d_o.at[1]))
        staged.append(pltpu.make_async_copy(conv_in.at[at], o_ref.at[h, key:], d_o.at[1]))
    for c in staged:
        c.start()
    barrier = pltpu.get_barrier_semaphore()
    for d in range(1, every):
        pl.semaphore_signal(
            barrier, inc=1, device_id=in_group(lax.rem(e_me + d, every)), device_id_type=MESH
        )
    for d in range(1, lines):
        pl.semaphore_signal(
            barrier, inc=1, device_id=along(lax.rem(q + d, lines)), device_id_type=MESH
        )
    pl.semaphore_wait(barrier, every - 1 + lines - 1)

    has_right, has_left = q + 1 < lines, q > 0
    right = along(lax.rem(q + 1, lines))
    left = along(lax.rem(q + lines - 1, lines))

    def moves(src, dst, send_r, send_l, recv, s):
        return (
            copy(src, dst.at[s], send_r.at[s], recv.at[s], right),
            copy(src, dst.at[s], send_l.at[s], recv.at[s], left),
        )

    def forward(src, dst, send_r, send_l, recv, s, to_right=True, to_left=True):
        go_right, go_left = moves(src, dst, send_r, send_l, recv, s)
        if to_right:
            pl.when(has_right)(go_right.start)
        if to_left:
            pl.when(has_left)(go_left.start)

    W = (gw, sr_w, sl_w, v_w)
    O = (go, sr_o, sl_o, v_o)

    def swaps(ref, dst, send, recv):
        found = []
        for j in range(1, heads):
            other = lax.rem(r + j, heads)
            found.append(
                copy(ref.at[other], dst, send.at[j], recv, (q * heads + other, t_me))
            )
        return found

    w_swaps = swaps(w_ref, gw.at[s_me], s_w, v_w.at[s_me])
    e_swaps = swaps(ed_ref, ge.at[r], s_e, v_e.at[r])
    o_swaps = swaps(o_ref, go.at[s_me], s_o, v_o.at[s_me])
    y, c = r // 2, lax.rem(r, 2)
    cc, yy, xx = 1 - c, 1 - y, 1 - t_me

    def slot(y, c, x):
        return (y * 2 + c) * groups + x

    core = (q * heads + y * 2 + cc, t_me)
    over_y = (q * heads + yy * 2 + c, t_me)
    over_x = (s_me, xx)
    over_xy = (q * heads + yy * 2 + c, xx)
    t_sends = [
        copy(tok_ref, tg.at[e_me], s_t.at[n], v_t.at[e_me], dev)
        for n, dev in enumerate((core, over_x, over_y, over_xy))
    ]
    t_passes = [
        copy(tg.at[e], tg.at[e], s_t.at[4 + n], v_t.at[e], core)
        for n, e in enumerate((slot(y, c, xx), slot(yy, c, t_me), slot(yy, c, xx)))
    ]
    pltpu.make_async_copy(w_ref.at[r], w_ref.at[r], d_w.at[r]).wait()
    forward(w_ref.at[r], *W, s_me)
    for j in range(1, heads):
        h = lax.rem(r + j, heads)
        pltpu.make_async_copy(w_ref.at[h], w_ref.at[h], d_w.at[h]).wait()
        w_swaps[j - 1].start()
    pltpu.make_async_copy(tok_in, tok_ref, d_o.at[0]).wait()
    for d in e_swaps + t_sends:
        d.start()
    pltpu.make_async_copy(o_ref, o_ref, d_o.at[1]).wait()
    for d in o_swaps:
        d.start()
    gw[s_me] = w_ref[r]
    go[s_me] = o_ref[r]
    ge[r] = ed_ref[r]

    def arrived(dst, recv, s):
        copy(dst.at[s], dst.at[s], s_p.at[0], recv.at[s], right).wait_recv()

    def relay_own(kind):
        for j in range(1, heads):
            s = q * heads + lax.rem(r + j, heads)
            arrived(kind[0], kind[3], s)
            forward(kind[0].at[s], *kind, s)

    step = 16

    def norm(e, src):
        def body(i, _):
            at = pl.ds(pl.multiple_of(i * step, step), step)
            x = src[at, :].astype(f32)
            normed[e, at, :] = (x * rms_scale(x) * gain_ref[...]).astype(bf16)
            return 0

        lax.fori_loop(0, rows // step, body, 0)

    def take(e):
        arrived(tg, v_t, e)
        norm(e, tg.at[e])

    def hand_on(n, e):
        arrived(tg, v_t, e)
        t_passes[n].start()

    by_x, by_y, by_xy = slot(y, c, xx), slot(yy, c, t_me), slot(yy, c, xx)
    chores = [
        lambda: norm(e_me, tok_ref),
        lambda: take(slot(y, cc, t_me)),
        lambda: hand_on(0, by_x),
        lambda: norm(by_x, tg.at[by_x]),
        lambda: hand_on(1, by_y),
        lambda: norm(by_y, tg.at[by_y]),
        lambda: take(slot(y, cc, xx)),
        lambda: take(slot(yy, cc, t_me)),
        lambda: hand_on(2, by_xy),
        lambda: norm(by_xy, tg.at[by_xy]),
        lambda: take(slot(yy, cc, xx)),
    ]

    def relay(kind, k, between):
        for j in range(heads):
            rr = lax.rem(r + j, heads)

            @pl.when(q >= k)
            def _():
                s = (q - k) * heads + rr
                arrived(kind[0], kind[3], s)
                forward(kind[0].at[s], *kind, s, to_left=False)

            @pl.when(q + k < lines)
            def _():
                s = (q + k) * heads + rr
                arrived(kind[0], kind[3], s)
                forward(kind[0].at[s], *kind, s, to_right=False)

            if between:
                between.pop(0)()

    def relay_inner(kind, k, inner):
        for j in range(heads):
            rr = lax.rem(r + j, heads)

            @pl.when(jnp.logical_and(q >= k, has_right == inner))
            def _():
                s = (q - k) * heads + rr
                arrived(kind[0], kind[3], s)
                forward(kind[0].at[s], *kind, s, to_left=False)

            @pl.when(jnp.logical_and(q + k < lines, has_left == inner))
            def _():
                s = (q + k) * heads + rr
                arrived(kind[0], kind[3], s)
                forward(kind[0].at[s], *kind, s, to_right=False)

    relay_own(W)
    for k in range(1, lines):
        relay(W, k, chores)
        if k == lines - 2:
            forward(o_ref.at[r], *O, s_me)
            relay_own(O)
    for k in range(1, lines):
        relay_inner(O, k, True)
    while chores:
        chores.pop(0)()

    depth = heads * w_ref.shape[1]
    tall = 2 * rows

    def project(i, _):
        at = pl.ds(pl.multiple_of(i * tall, tall), tall)
        acc = jnp.zeros((tall, 7 * key), f32)
        for p in range(lines):
            x = normed[pl.ds(i * 2, 2), :, pl.ds(p * depth, depth)].reshape(tall, depth)
            w = gw[pl.ds(p * heads, heads)].reshape(depth, 7 * key)
            acc = acc + jnp.dot(x, w, preferred_element_type=f32)
        proj[at, :] = acc.astype(bf16)
        return 0

    lax.fori_loop(0, length // tall, project, 0)
    for j in range(1, heads):
        arrived(ge, v_e, lax.rem(r + j, heads))

    def column(at, number):
        return proj[at, number * key : (number + 1) * key].astype(f32)

    pad = 8
    blocks = length // block
    per = blocks // heads
    tri = (
        lax.broadcasted_iota(jnp.int32, (block, block), 0)
        >= lax.broadcasted_iota(jnp.int32, (block, block), 1)
    ).astype(f32)
    wide = (
        lax.broadcasted_iota(jnp.int32, (block, key), 0)
        >= lax.broadcasted_iota(jnp.int32, (block, key), 1)
    ).astype(f32)
    gap = gap_ref[pl.ds(r, 1), :]
    packet[...] = jnp.zeros_like(packet)

    def advance(b, _):
        at = pl.ds(pl.multiple_of(b * block, block), block)
        query = column(at, 0)
        query = query * sigmoid(query)
        write = gap * sigmoid(-column(at, 1))
        values = column(at, 2)
        extra = ge[b // per, pl.ds(lax.rem(b, per), 1), :]
        run = high_dot(tri, jnp.log1p(-write), ((1,), (0,))) + jnp.sum(
            wide * extra, axis=1, keepdims=True
        )
        final = run[block - 1 : block, :]
        middle = 0.5 * final
        scores = tri * high_dot(
            query * jnp.exp(run - middle), write * jnp.exp(middle - run), ((1,), (1,))
        )
        before = packet[:key, :]
        offset = packet[key : key + 1, :]
        lift = query * jnp.exp(run)
        mixed[at, :] = high_dot(scores, values, ((1,), (0,))) + high_dot(
            lift, before, ((1,), (1,))
        )
        lifted[at, :] = lift * jnp.exp(offset)
        packet[:key, :] = before * jnp.exp(final) + high_dot(
            values, write * jnp.exp(final - run), ((0,), (0,))
        )
        packet[key : key + pad, :] = jnp.broadcast_to(offset + final, (pad, key))
        gated[pl.ds(pl.multiple_of(b * block + pad, pad), block), :] = column(at, 5) * column(at, 6)
        return 0

    lax.fori_loop(0, blocks, advance, 0)
    packet[key + pad : key + 2 * pad, :] = gated[length : length + pad, :]

    def packet_to(d):
        return copy(
            packet, packets.at[q], s_p.at[d], v_p.at[q], along(lax.rem(q + d, lines))
        )

    for d in range(1, lines):
        pl.when(q + d < lines)(packet_to(d).start)
    state[...] = start_ref[r].T
    gated[:pad, :] = jnp.zeros((pad, key), f32)
    for p in range(lines - 1):

        @pl.when(p < q)
        def _():
            arrived(packets, v_p, p)
            state[...] = state[...] * jnp.exp(packets[p, key : key + 1, :]) + packets[p, :key, :]

        @pl.when(p + 1 == q)
        def _():
            gated[:pad, :] = packets[p, key + pad : key + 2 * pad, :]

    for k in range(1, lines):
        relay_inner(O, k, False)
    taps = taps_ref[:, pl.ds(pl.multiple_of(r * key, key), key)]
    span = o_ref.shape[2]
    width = span * heads * lines
    half = width // 2

    def finish(e):
        start = pl.multiple_of(e * rows, rows)
        at = pl.ds(start, rows)
        m = mixed[at, :] + high_dot(lifted[at, :], state[...], ((1,), (1,)))
        gate = column(at, 3)
        rec = m * rms_scale(m) * sgain_ref[...] * (gate * sigmoid(gate))
        near = gated[pl.ds(start, rows + pad), :]
        conv = (
            taps[0:1] * near[pad - 2 : pad - 2 + rows]
            + taps[1:2] * near[pad - 1 : pad - 1 + rows]
            + taps[2:3] * near[pad : pad + rows]
        )
        left_side = jnp.concatenate(
            [rec.astype(bf16), (column(at, 4) * conv).astype(bf16)], axis=1
        )
        for p in range(heads * lines // 2):
            w = jnp.concatenate([go[2 * p], go[2 * p + 1]], axis=1)
            part[e, :, 2 * span * p : 2 * span * (p + 1)] = jnp.dot(
                left_side, w, preferred_element_type=f32
            ).astype(bf16)

    lo, hi = pl.ds(0, half), pl.ds(half, half)
    order = ((yy, xx), (yy, t_me), (y, xx), (y, t_me))
    first = []
    for a, b in order:
        n = 2 * a + b
        finish(slot(a, cc, b))
        first.append(copy(part.at[slot(a, cc, b)], r0.at[n], s_x0.at[n], v_x0.at[n], core))
        first[-1].start()

    def add(e, cols, other):
        return part[e, :, cols].astype(f32) + other.astype(f32)

    def arrived_hi(b):
        copy(r1b.at[b], r1b.at[b], s_p.at[0], v_x1.at[2 + b], right).wait_recv()

    def to_y(b):
        return copy(part.at[slot(yy, c, b), :, lo], r1a.at[b], s_x1.at[b], v_x1.at[b], over_y)

    def to_x(b):
        return copy(
            part.at[slot(b, c, xx), :, hi], r1b.at[b], s_x1.at[2 + b], v_x1.at[2 + b], over_x
        )

    second = [to_y(xx), to_x(yy), to_y(t_me), to_x(y)]
    sends = [second[:2], second[2:3], second[3:], []]
    for (a, b), ready, d in zip(order, sends, first):
        e = slot(a, c, b)
        finish(e)
        d.wait_recv()
        part[e] = (part[e].astype(f32) + r0[2 * a + b].astype(f32)).astype(bf16)
        for s in ready:
            s.start()
    third = [
        copy(part.at[slot(y, c, xx), :, lo], r2.at[0], s_x2.at[0], v_x2.at[0], over_x),
        copy(part.at[slot(yy, c, t_me), :, hi], r2.at[1], s_x2.at[1], v_x2.at[1], over_y),
    ]
    arrived(r1a, v_x1, xx)
    part[slot(y, c, xx), :, lo] = add(slot(y, c, xx), lo, r1a[xx]).astype(bf16)
    third[0].start()
    arrived_hi(yy)
    part[slot(yy, c, t_me), :, hi] = add(slot(yy, c, t_me), hi, r1b[yy]).astype(bf16)
    third[1].start()
    mine = slot(y, c, t_me)
    arrived(r1a, v_x1, t_me)
    arrived_hi(y)
    for d in third:
        d.wait_recv()
    out_ref[:, lo] = (add(mine, lo, r1a[t_me]) + r2[0].astype(f32)).astype(bf16)
    out_ref[:, hi] = (add(mine, hi, r1b[y]) + r2[1].astype(f32)).astype(bf16)
    for d in first + second + third + t_passes:
        d.wait_send()

    for d in w_swaps + e_swaps + o_swaps + t_sends:
        d.wait_send()
    for d in range(1, lines):
        pl.when(q + d < lines)(packet_to(d).wait_send)

    for kind in (W, O):
        for p in range(lines):
            for j in range(heads):
                s = p * heads + j
                go_right, go_left = moves(kind[0].at[s], *kind, s)
                pl.when(jnp.logical_and(has_right, p <= q))(go_right.wait_send)
                pl.when(jnp.logical_and(has_left, p >= q))(go_left.wait_send)


def fused(heads, lines, groups, *args):
    (tokens, norm_gain, w_query, w_forget, w_input, w_outgate, w_bgate, w_cgate, w_value,
     floor_gap, extra_decay, start_state, state_gain, conv_taps, out_rec, out_conv) = args
    rows, model = tokens.shape
    depth = w_query.shape[0]
    key = floor_gap.shape[1]
    span = out_rec.shape[1]
    every = heads * groups
    length = every * rows
    sp = heads * lines
    pad = 8

    weights = (w_query, w_forget, w_input, w_outgate, w_bgate, w_cgate, w_value)
    per = extra_decay.shape[0] // BLOCK
    extra = extra_decay.T.reshape(heads, per, BLOCK)
    extra = jnp.pad(extra, ((0, 0), (0, pad - per), (0, key - BLOCK)))
    dma = pltpu.SemaphoreType.DMA
    half = model // 2
    scratch = [
        pltpu.VMEM((rows, model), bf16),
        pltpu.VMEM((heads, depth, 7 * key), bf16),
        pltpu.VMEM((heads, 2 * key, span), bf16),
        pltpu.VMEM((every, rows, model), bf16),
        pltpu.VMEM((every, rows, model), bf16),
        pltpu.VMEM((sp, depth, 7 * key), bf16),
        pltpu.VMEM((sp, 2 * key, span), bf16),
        pltpu.VMEM((heads, pad, key), f32),
        pltpu.VMEM((length, 7 * key), bf16),
        pltpu.VMEM((length + pad, key), f32),
        pltpu.VMEM((length, key), f32),
        pltpu.VMEM((length, key), f32),
        pltpu.VMEM((key + 2 * pad, key), f32),
        pltpu.VMEM((lines, key + 2 * pad, key), f32),
        pltpu.VMEM((key, key), f32),
        pltpu.VMEM((every, rows, model), bf16),
        pltpu.VMEM((every // 2, rows, model), bf16),
        pltpu.VMEM((2, rows, half), bf16),
        pltpu.VMEM((2, rows, half), bf16),
        pltpu.VMEM((2, rows, half), bf16),
        dma((heads,)), dma((heads,)), dma((heads,)), dma((every,)), dma((lines,)),
        dma((sp,)), dma((sp,)), dma((sp,)), dma((sp,)),
        dma((sp,)), dma((sp,)), dma((heads,)), dma((every,)), dma((lines,)),
        dma((4,)), dma((4,)), dma((4,)), dma((4,)), dma((2,)), dma((2,)),
        dma((heads,)), dma((2,)),
    ]
    hbm = pl.BlockSpec(memory_space=pl.ANY)
    vmem = pl.BlockSpec(memory_space=pltpu.VMEM)
    return pl.pallas_call(
        functools.partial(fused_kernel, heads, lines, groups, BLOCK),
        out_shape=jax.ShapeDtypeStruct((rows, model), bf16),
        in_specs=[hbm, vmem, (hbm,) * 7, hbm, hbm] + [vmem] * 5,
        out_specs=pl.BlockSpec(memory_space=pltpu.VMEM),
        scratch_shapes=scratch,
        compiler_params=pltpu.CompilerParams(
            collective_id=0, has_side_effects=True, vmem_limit_bytes=60 * 1024 * 1024
        ),
        name="mixer",
    )(
        tokens, norm_gain[None], weights, out_rec, out_conv, floor_gap, extra, start_state,
        state_gain[None], conv_taps,
    )


def per_device(sp, tp, *args):
    heads = args[9].shape[0]
    fits = (
        heads == 4 and tp == 2 and sp % heads == 0
        and args[14].shape[1] % 128 == 0
        and args[13].shape[1] == heads * args[9].shape[1]
        and args[10].shape[0] % BLOCK == 0
    )
    if not fits:
        return on_device(*args)
    return fused(heads, sp // heads, tp, *args)


def solution(mesh):
    placed = (
        P(("sp", "tp"), None),
        P(),
        P("sp", "tp"),
        P("sp", "tp"),
        P("sp", "tp"),
        P("sp", "tp"),
        P("sp", "tp"),
        P("sp", "tp"),
        P("sp", "tp"),
        P("tp", None),
        P("sp", "tp"),
        P("tp", None, None),
        P(),
        P(None, "tp"),
        P("tp", "sp"),
        P("tp", "sp"),
    )
    return jax.shard_map(
        functools.partial(per_device, mesh.shape["sp"], mesh.shape["tp"]), mesh=mesh, in_specs=placed, out_specs=P(("sp", "tp"), None), check_vma=False
    )
```

```python
import functools

import jax
import jax.numpy as jnp
from jax import lax
from jax.experimental import pallas as pl
from jax.experimental.pallas import tpu as pltpu
from jax.sharding import PartitionSpec as P

BLOCK = 64


eps = 1e-06
highest_precision = lax.Precision.HIGHEST


def prefix(value, axis, join, neutral):
    count, mine = (lax.axis_size(axis), lax.axis_index(axis))
    pieces = jax.tree.map(lambda part: lax.all_gather(part, axis), value)
    so_far = jax.tree.map(
        lambda part, zero: jnp.full_like(part, 0) + jnp.asarray(zero, part.dtype), value, neutral
    )

    def hop(position, so_far):
        longer = join(so_far, jax.tree.map(lambda part: part[position], pieces))
        return jax.tree.map(lambda new, old: jnp.where(position < mine, new, old), longer, so_far)

    return lax.fori_loop(0, count - 1, hop, so_far)


def shifted(block, axis, distance):
    devices = range(lax.axis_size(axis))
    route = [(i - distance, i) for i in devices if i - distance in devices]
    return lax.ppermute(block, axis, route)


def rms_scale(values):
    return lax.rsqrt(jnp.mean(values * values, axis=-1, keepdims=True) + eps)


def local_blocks(queries, write_in, inputs, log_keep, block_len):
    length, head_count, address_feature_count = queries.shape
    value_dim = inputs.shape[-1]
    blocks_count = length // block_len

    def blocked(tensor):
        return tensor.reshape(blocks_count, block_len, head_count, tensor.shape[-1]).transpose(
            0, 2, 1, 3
        )

    def unblock(tensor):
        return tensor.transpose(0, 2, 1, 3).reshape(length, head_count, tensor.shape[-1])

    causal = (jnp.arange(block_len)[:, None] >= jnp.arange(block_len)[None, :])[None, :, :, None]

    def advance(carried, pieces):
        memory_state, offset = carried
        query_block, write_blk, input_block, keep_blk = pieces
        running_state = jnp.cumsum(keep_blk, axis=1)
        spread = running_state[:, :, None, :] - running_state[:, None, :, :]
        decays = jnp.where(causal, jnp.exp(jnp.minimum(spread, 0.0)), 0.0)
        scores = jnp.sum(query_block[:, :, None, :] * write_blk[:, None, :, :] * decays, axis=-1)
        final_output = jnp.einsum(
            "qcp,qpi->qci",
            query_block * jnp.exp(running_state),
            memory_state,
            precision=highest_precision,
        )
        final_output = final_output + jnp.einsum(
            "hts,hsv->htv", scores, input_block, precision=highest_precision
        )
        lifted_state = query_block * jnp.exp(running_state + offset[:, None, :])
        final_state = running_state[:, -1, :]
        weighted_value = write_blk * jnp.exp(final_state[:, None, :] - running_state)
        memory_state = memory_state * jnp.exp(final_state)[:, :, None] + jnp.einsum(
            "euz,eul->ezl", weighted_value, input_block, precision=highest_precision
        )
        return ((memory_state, offset + final_state), (final_output, lifted_state))

    initial = (
        jnp.zeros((head_count, address_feature_count, value_dim), jnp.float32),
        jnp.zeros((head_count, address_feature_count), jnp.float32),
    )
    finals, outputs = lax.scan(
        advance, initial, (blocked(queries), blocked(write_in), blocked(inputs), blocked(log_keep))
    )
    return (unblock(outputs[0]), unblock(outputs[1]), finals[0], jnp.exp(finals[1]))


def chain(earlier, later):
    return (earlier[0] * later[0], earlier[1] * later[0][:, :, None] + later[1])


def on_device(
    tokens,
    norm_gain,
    w_query,
    w_forget,
    w_input,
    w_outgate,
    w_bgate,
    w_cgate,
    w_value,
    floor_gap,
    extra_decay,
    start_state,
    state_gain,
    conv_taps,
    out_rec,
    out_conv,
):
    tokens_f = tokens.astype(jnp.float32)
    normed = (tokens_f * rms_scale(tokens_f) * norm_gain).astype(jnp.bfloat16)
    weights = (w_query, w_forget, w_input, w_outgate, w_bgate, w_cgate, w_value)
    whole_weights = (
        lax.all_gather(w_query, "sp", axis=0, tiled=True),
        lax.all_gather(w_forget, "sp", axis=0, tiled=True),
        lax.all_gather(w_input, "sp", axis=0, tiled=True),
        lax.all_gather(w_outgate, "sp", axis=0, tiled=True),
        lax.all_gather(w_bgate, "sp", axis=0, tiled=True),
        lax.all_gather(w_cgate, "sp", axis=0, tiled=True),
        lax.all_gather(w_value, "sp", axis=0, tiled=True),
    )

    def project(shard_rows):
        return jnp.concatenate(
            [
                jnp.dot(shard_rows, matrix, preferred_element_type=jnp.float32).astype(jnp.bfloat16)
                for matrix in whole_weights
            ],
            axis=1,
        )

    joined = project(lax.all_gather(normed, "tp", axis=0, tiled=True))
    borders = [0]
    for matrix in weights:
        borders.append(borders[-1] + matrix.shape[1])
    projected = [joined[:, borders[number] : borders[number + 1]] for number in range(len(weights))]
    query_raw, forget_raw, input_raw, outgate_raw, bgate_raw, cgate_raw, value_raw = projected
    length = query_raw.shape[0]
    head_count, address_feature_count = floor_gap.shape
    value_dim = start_state.shape[2]
    queries = jax.nn.silu(query_raw.astype(jnp.float32)).reshape(
        length, head_count, address_feature_count
    )
    write_in = floor_gap[None] * jax.nn.sigmoid(-forget_raw.astype(jnp.float32)).reshape(
        length, head_count, address_feature_count
    )
    log_keep = jnp.log1p(-write_in) + extra_decay[:, :, None]
    inputs = input_raw.astype(jnp.float32).reshape(length, head_count, value_dim)
    output_list, lifted_state, memory_state, kept = local_blocks(
        queries, write_in, inputs, log_keep, BLOCK
    )
    before_keep, before_memory = prefix(
        (kept, memory_state), "sp", chain, (jnp.ones_like(kept), jnp.zeros_like(memory_state))
    )
    carried_hidden_prior = start_state * before_keep[:, :, None] + before_memory
    blended_state = output_list + jnp.einsum(
        "sqa,qar->sqr", lifted_state, carried_hidden_prior, precision=highest_precision
    )
    gate_out = jax.nn.silu(outgate_raw.astype(jnp.float32)).reshape(length, head_count, value_dim)
    rec_out = (
        (blended_state * rms_scale(blended_state) * state_gain * gate_out)
        .reshape(length, head_count * value_dim)
        .astype(jnp.bfloat16)
    )
    rim_rows = jnp.stack([cgate_raw[length - 2 :], value_raw[length - 2 :]])
    before_rim = shifted(rim_rows, "sp", 1)
    convolution_gate_widened = jnp.concatenate([before_rim[0], cgate_raw], axis=0).astype(
        jnp.float32
    )
    value_ext = jnp.concatenate([before_rim[1], value_raw], axis=0).astype(jnp.float32)
    gated = convolution_gate_widened * value_ext
    conv_out = (
        conv_taps[0] * gated[:length]
        + conv_taps[1] * gated[1 : length + 1]
        + conv_taps[2] * gated[2:]
    )
    short_out = (bgate_raw.astype(jnp.float32) * conv_out).astype(jnp.bfloat16)
    rec_weight, conv_weight = (
        lax.all_gather(out_rec, "sp", axis=1, tiled=True),
        lax.all_gather(out_conv, "sp", axis=1, tiled=True),
    )
    product = jnp.dot(rec_out, rec_weight, preferred_element_type=jnp.float32)
    return lax.psum_scatter(
        (product + jnp.dot(short_out, conv_weight, preferred_element_type=jnp.float32)).astype(
            jnp.bfloat16
        ),
        "tp",
        scatter_dimension=0,
        tiled=True,
    )


MESH = pl.DeviceIdType.MESH
f32, bf16 = jnp.float32, jnp.bfloat16


def high_dot(a, b, dims):
    return lax.dot_general(
        a, b, (dims, ((), ())), precision=highest_precision, preferred_element_type=f32
    )


def sigmoid(v):
    return 1.0 / (1.0 + jnp.exp(-v))


def fused_kernel(
    heads,
    lines,
    groups,
    block,
    tok_in,
    gain_ref,
    w_ins,
    rec_in,
    conv_in,
    gap_ref,
    ed_ref,
    start_ref,
    sgain_ref,
    taps_ref,
    out_ref,
    tok_ref,
    w_ref,
    o_ref,
    normed,
    tg,
    gw,
    go,
    ge,
    proj,
    gated,
    runs,
    befores,
    packet,
    packets,
    state,
    part,
    r0,
    r1a,
    r1b,
    r2,
    s_w,
    s_o,
    s_e,
    s_t,
    s_p,
    sr_w,
    sl_w,
    sr_o,
    sl_o,
    v_w,
    v_o,
    v_e,
    v_t,
    v_p,
    s_x0,
    v_x0,
    s_x1,
    v_x1,
    s_x2,
    v_x2,
    d_w,
    d_o,
):
    s_me, t_me = lax.axis_index("sp"), lax.axis_index("tp")
    q, r = s_me // heads, lax.rem(s_me, heads)
    e_me = r * groups + t_me
    every = heads * groups
    rows = tok_ref.shape[0]
    key = w_ref.shape[2] // 7
    length = every * rows

    def copy(src, dst, send, recv, dev):
        return pltpu.make_async_remote_copy(
            src_ref=src, dst_ref=dst, send_sem=send, recv_sem=recv, device_id=dev,
            device_id_type=MESH,
        )

    def in_group(e):
        return (q * heads + e // groups, lax.rem(e, groups))

    def along(p):
        return (p * heads + r, t_me)

    staged = []
    for j in range(heads):
        h = lax.rem(r + j, heads)
        for number, w_in in enumerate(w_ins):
            staged.append(
                pltpu.make_async_copy(
                    w_in.at[:, pl.ds(pl.multiple_of(h * key, key), key)],
                    w_ref.at[h, :, number * key : (number + 1) * key],
                    d_w.at[h],
                )
            )
    staged.append(pltpu.make_async_copy(tok_in, tok_ref, d_o.at[0]))
    for h in range(heads):
        at = pl.ds(h * key, key)
        staged.append(pltpu.make_async_copy(rec_in.at[at], o_ref.at[h, :key], d_o.at[1]))
        staged.append(pltpu.make_async_copy(conv_in.at[at], o_ref.at[h, key:], d_o.at[1]))
    for c in staged:
        c.start()
    barrier = pltpu.get_barrier_semaphore()
    for d in range(1, every):
        pl.semaphore_signal(
            barrier, inc=1, device_id=in_group(lax.rem(e_me + d, every)), device_id_type=MESH
        )
    for d in range(1, lines):
        pl.semaphore_signal(
            barrier, inc=1, device_id=along(lax.rem(q + d, lines)), device_id_type=MESH
        )
    pl.semaphore_wait(barrier, every - 1 + lines - 1)

    has_right, has_left = q + 1 < lines, q > 0
    right = along(lax.rem(q + 1, lines))
    left = along(lax.rem(q + lines - 1, lines))

    def moves(src, dst, send_r, send_l, recv, s):
        return (
            copy(src, dst.at[s], send_r.at[s], recv.at[s], right),
            copy(src, dst.at[s], send_l.at[s], recv.at[s], left),
        )

    def forward(src, dst, send_r, send_l, recv, s, to_right=True, to_left=True):
        go_right, go_left = moves(src, dst, send_r, send_l, recv, s)
        if to_right:
            pl.when(has_right)(go_right.start)
        if to_left:
            pl.when(has_left)(go_left.start)

    W = (gw, sr_w, sl_w, v_w)
    O = (go, sr_o, sl_o, v_o)

    def swaps(ref, dst, send, recv):
        found = []
        for j in range(1, heads):
            other = lax.rem(r + j, heads)
            found.append(
                copy(ref.at[other], dst, send.at[j], recv, (q * heads + other, t_me))
            )
        return found

    w_swaps = swaps(w_ref, gw.at[s_me], s_w, v_w.at[s_me])
    e_swaps = swaps(ed_ref, ge.at[r], s_e, v_e.at[r])
    o_swaps = swaps(o_ref, go.at[s_me], s_o, v_o.at[s_me])
    y, c = r // 2, lax.rem(r, 2)
    cc, yy, xx = 1 - c, 1 - y, 1 - t_me

    def slot(y, c, x):
        return (y * 2 + c) * groups + x

    core = (q * heads + y * 2 + cc, t_me)
    over_y = (q * heads + yy * 2 + c, t_me)
    over_x = (s_me, xx)
    over_xy = (q * heads + yy * 2 + c, xx)
    t_sends = [
        copy(tok_ref, tg.at[e_me], s_t.at[n], v_t.at[e_me], dev)
        for n, dev in enumerate((core, over_x, over_y, over_xy))
    ]
    t_passes = [
        copy(tg.at[e], tg.at[e], s_t.at[4 + n], v_t.at[e], core)
        for n, e in enumerate((slot(y, c, xx), slot(yy, c, t_me), slot(yy, c, xx)))
    ]
    pltpu.make_async_copy(w_ref.at[r], w_ref.at[r], d_w.at[r]).wait()
    forward(w_ref.at[r], *W, s_me)
    for j in range(1, heads):
        h = lax.rem(r + j, heads)
        pltpu.make_async_copy(w_ref.at[h], w_ref.at[h], d_w.at[h]).wait()
        w_swaps[j - 1].start()
    pltpu.make_async_copy(tok_in, tok_ref, d_o.at[0]).wait()
    for d in e_swaps + t_sends:
        d.start()
    pltpu.make_async_copy(o_ref, o_ref, d_o.at[1]).wait()
    for d in o_swaps:
        d.start()
    gw[s_me] = w_ref[r]
    go[s_me] = o_ref[r]
    ge[r] = ed_ref[r]

    def arrived(dst, recv, s):
        copy(dst.at[s], dst.at[s], s_p.at[0], recv.at[s], right).wait_recv()

    def relay_own(kind):
        for j in range(1, heads):
            s = q * heads + lax.rem(r + j, heads)
            arrived(kind[0], kind[3], s)
            forward(kind[0].at[s], *kind, s)

    step = 16

    def norm(e, src):
        def body(i, _):
            at = pl.ds(pl.multiple_of(i * step, step), step)
            x = src[at, :].astype(f32)
            normed[e, at, :] = (x * rms_scale(x) * gain_ref[...]).astype(bf16)
            return 0

        lax.fori_loop(0, rows // step, body, 0)

    def take(e):
        arrived(tg, v_t, e)
        norm(e, tg.at[e])

    def hand_on(n, e):
        arrived(tg, v_t, e)
        t_passes[n].start()

    by_x, by_y, by_xy = slot(y, c, xx), slot(yy, c, t_me), slot(yy, c, xx)
    chores = [
        lambda: norm(e_me, tok_ref),
        lambda: take(slot(y, cc, t_me)),
        lambda: hand_on(0, by_x),
        lambda: norm(by_x, tg.at[by_x]),
        lambda: hand_on(1, by_y),
        lambda: norm(by_y, tg.at[by_y]),
        lambda: take(slot(y, cc, xx)),
        lambda: take(slot(yy, cc, t_me)),
        lambda: hand_on(2, by_xy),
        lambda: norm(by_xy, tg.at[by_xy]),
        lambda: take(slot(yy, cc, xx)),
    ]

    def relay(kind, k, between):
        for j in range(heads):
            rr = lax.rem(r + j, heads)

            @pl.when(q >= k)
            def _():
                s = (q - k) * heads + rr
                arrived(kind[0], kind[3], s)
                forward(kind[0].at[s], *kind, s, to_left=False)

            @pl.when(q + k < lines)
            def _():
                s = (q + k) * heads + rr
                arrived(kind[0], kind[3], s)
                forward(kind[0].at[s], *kind, s, to_right=False)

            if between:
                between.pop(0)()

    def relay_inner(kind, k, inner):
        for j in range(heads):
            rr = lax.rem(r + j, heads)

            @pl.when(jnp.logical_and(q >= k, has_right == inner))
            def _():
                s = (q - k) * heads + rr
                arrived(kind[0], kind[3], s)
                forward(kind[0].at[s], *kind, s, to_left=False)

            @pl.when(jnp.logical_and(q + k < lines, has_left == inner))
            def _():
                s = (q + k) * heads + rr
                arrived(kind[0], kind[3], s)
                forward(kind[0].at[s], *kind, s, to_right=False)

    relay_own(W)
    for k in range(1, lines):
        relay(W, k, chores)
        if k == lines - 2:
            forward(o_ref.at[r], *O, s_me)
            relay_own(O)
    for k in range(1, lines):
        relay_inner(O, k, True)
    while chores:
        chores.pop(0)()

    depth = heads * w_ref.shape[1]
    tall = 2 * rows

    def project(i, _):
        at = pl.ds(pl.multiple_of(i * tall, tall), tall)
        acc = jnp.zeros((tall, 7 * key), f32)
        for p in range(lines):
            x = normed[pl.ds(i * 2, 2), :, pl.ds(p * depth, depth)].reshape(tall, depth)
            w = gw[pl.ds(p * heads, heads)].reshape(depth, 7 * key)
            acc = acc + jnp.dot(x, w, preferred_element_type=f32)
        proj[at, :] = acc.astype(bf16)
        return 0

    lax.fori_loop(0, length // tall, project, 0)
    for j in range(1, heads):
        arrived(ge, v_e, lax.rem(r + j, heads))

    def column(at, number):
        return proj[at, number * key : (number + 1) * key].astype(f32)

    pad = 8
    blocks = length // block
    per = blocks // heads
    tri = (
        lax.broadcasted_iota(jnp.int32, (block, block), 0)
        >= lax.broadcasted_iota(jnp.int32, (block, block), 1)
    ).astype(f32)
    wide = (
        lax.broadcasted_iota(jnp.int32, (block, key), 0)
        >= lax.broadcasted_iota(jnp.int32, (block, key), 1)
    ).astype(f32)
    gap = gap_ref[pl.ds(r, 1), :]
    packet[...] = jnp.zeros_like(packet)

    def writing(at):
        return gap * sigmoid(-column(at, 1))

    def advance(b, _):
        at = pl.ds(pl.multiple_of(b * block, block), block)
        write = writing(at)
        extra = ge[b // per, pl.ds(lax.rem(b, per), 1), :]
        run = high_dot(tri, jnp.log1p(-write), ((1,), (0,))) + jnp.sum(
            wide * extra, axis=1, keepdims=True
        )
        final = run[block - 1 : block, :]
        runs[at, :] = run
        before = packet[: key + pad, :]
        befores[b] = before
        packet[:key, :] = before[:key] * jnp.exp(final) + high_dot(
            column(at, 2), write * jnp.exp(final - run), ((0,), (0,))
        )
        packet[key : key + pad, :] = before[key:] + final
        gated[pl.ds(pl.multiple_of(b * block + pad, pad), block), :] = column(at, 5) * column(at, 6)
        return 0

    lax.fori_loop(0, blocks, advance, 0, unroll=4)
    packet[key + pad : key + 2 * pad, :] = gated[length : length + pad, :]

    def packet_to(d):
        return copy(
            packet, packets.at[q], s_p.at[d], v_p.at[q], along(lax.rem(q + d, lines))
        )

    for d in range(1, lines):
        pl.when(q + d < lines)(packet_to(d).start)
    state[...] = start_ref[r].T
    gated[:pad, :] = jnp.zeros((pad, key), f32)
    for p in range(lines - 1):

        @pl.when(p < q)
        def _():
            arrived(packets, v_p, p)
            state[...] = state[...] * jnp.exp(packets[p, key : key + 1, :]) + packets[p, :key, :]

        @pl.when(p + 1 == q)
        def _():
            gated[:pad, :] = packets[p, key + pad : key + 2 * pad, :]

    for k in range(1, lines):
        relay_inner(O, k, False)
    taps = taps_ref[:, pl.ds(pl.multiple_of(r * key, key), key)]
    span = o_ref.shape[2]
    width = span * heads * lines
    half = width // 2

    def finish(e):
        start = pl.multiple_of(e * rows, rows)
        at = pl.ds(start, rows)
        mixed = []
        for u in range(rows // block):
            here = pl.ds(pl.multiple_of(start + u * block, block), block)
            query = column(here, 0)
            query = query * sigmoid(query)
            run = runs[here, :]
            middle = 0.5 * run[block - 1 : block, :]
            scores = tri * high_dot(
                query * jnp.exp(run - middle), writing(here) * jnp.exp(middle - run), ((1,), (1,))
            )
            before = befores[e * (rows // block) + u]
            whole = before[:key] + state[...] * jnp.exp(before[key : key + 1])
            mixed.append(
                high_dot(scores, column(here, 2), ((1,), (0,)))
                + high_dot(query * jnp.exp(run), whole, ((1,), (1,)))
            )
        m = jnp.concatenate(mixed, axis=0)
        gate = column(at, 3)
        rec = m * rms_scale(m) * sgain_ref[...] * (gate * sigmoid(gate))
        near = gated[pl.ds(start, rows + pad), :]
        conv = (
            taps[0:1] * near[pad - 2 : pad - 2 + rows]
            + taps[1:2] * near[pad - 1 : pad - 1 + rows]
            + taps[2:3] * near[pad : pad + rows]
        )
        left_side = jnp.concatenate(
            [rec.astype(bf16), (column(at, 4) * conv).astype(bf16)], axis=1
        )
        for p in range(heads * lines // 2):
            w = jnp.concatenate([go[2 * p], go[2 * p + 1]], axis=1)
            part[e, :, 2 * span * p : 2 * span * (p + 1)] = jnp.dot(
                left_side, w, preferred_element_type=f32
            ).astype(bf16)

    lo, hi = pl.ds(0, half), pl.ds(half, half)
    order = ((yy, xx), (yy, t_me), (y, xx), (y, t_me))
    first = []

    def add(e, cols, other):
        return part[e, :, cols].astype(f32) + other.astype(f32)

    def arrived_hi(b):
        copy(r1b.at[b], r1b.at[b], s_p.at[0], v_x1.at[2 + b], right).wait_recv()

    def to_y(b):
        return copy(part.at[slot(yy, c, b), :, lo], r1a.at[b], s_x1.at[b], v_x1.at[b], over_y)

    def to_x(b):
        return copy(
            part.at[slot(b, c, xx), :, hi], r1b.at[b], s_x1.at[2 + b], v_x1.at[2 + b], over_x
        )

    second = [to_y(xx), to_x(yy), to_y(t_me), to_x(y)]
    sends = [second[:2], second[2:3], second[3:], []]
    for (a, b), ready in zip(order, sends):
        e, n = slot(a, c, b), 2 * a + b
        finish(slot(a, cc, b))
        d = copy(part.at[slot(a, cc, b)], r0.at[n], s_x0.at[n], v_x0.at[n], core)
        d.start()
        first.append(d)
        finish(e)
        d.wait_recv()
        part[e] = (part[e].astype(f32) + r0[2 * a + b].astype(f32)).astype(bf16)
        for s in ready:
            s.start()
    third = [
        copy(part.at[slot(y, c, xx), :, lo], r2.at[0], s_x2.at[0], v_x2.at[0], over_x),
        copy(part.at[slot(yy, c, t_me), :, hi], r2.at[1], s_x2.at[1], v_x2.at[1], over_y),
    ]
    arrived(r1a, v_x1, xx)
    part[slot(y, c, xx), :, lo] = add(slot(y, c, xx), lo, r1a[xx]).astype(bf16)
    third[0].start()
    arrived_hi(yy)
    part[slot(yy, c, t_me), :, hi] = add(slot(yy, c, t_me), hi, r1b[yy]).astype(bf16)
    third[1].start()
    mine = slot(y, c, t_me)
    arrived(r1a, v_x1, t_me)
    arrived_hi(y)
    for d in third:
        d.wait_recv()
    out_ref[:, lo] = (add(mine, lo, r1a[t_me]) + r2[0].astype(f32)).astype(bf16)
    out_ref[:, hi] = (add(mine, hi, r1b[y]) + r2[1].astype(f32)).astype(bf16)
    for d in first + second + third + t_passes:
        d.wait_send()

    for d in w_swaps + e_swaps + o_swaps + t_sends:
        d.wait_send()
    for d in range(1, lines):
        pl.when(q + d < lines)(packet_to(d).wait_send)

    for kind in (W, O):
        for p in range(lines):
            for j in range(heads):
                s = p * heads + j
                go_right, go_left = moves(kind[0].at[s], *kind, s)
                pl.when(jnp.logical_and(has_right, p <= q))(go_right.wait_send)
                pl.when(jnp.logical_and(has_left, p >= q))(go_left.wait_send)


def fused(heads, lines, groups, *args):
    (tokens, norm_gain, w_query, w_forget, w_input, w_outgate, w_bgate, w_cgate, w_value,
     floor_gap, extra_decay, start_state, state_gain, conv_taps, out_rec, out_conv) = args
    rows, model = tokens.shape
    depth = w_query.shape[0]
    key = floor_gap.shape[1]
    span = out_rec.shape[1]
    every = heads * groups
    length = every * rows
    sp = heads * lines
    pad = 8

    weights = (w_query, w_forget, w_input, w_outgate, w_bgate, w_cgate, w_value)
    per = extra_decay.shape[0] // BLOCK
    extra = extra_decay.T.reshape(heads, per, BLOCK)
    extra = jnp.pad(extra, ((0, 0), (0, pad - per), (0, key - BLOCK)))
    dma = pltpu.SemaphoreType.DMA
    half = model // 2
    scratch = [
        pltpu.VMEM((rows, model), bf16),
        pltpu.VMEM((heads, depth, 7 * key), bf16),
        pltpu.VMEM((heads, 2 * key, span), bf16),
        pltpu.VMEM((every, rows, model), bf16),
        pltpu.VMEM((every, rows, model), bf16),
        pltpu.VMEM((sp, depth, 7 * key), bf16),
        pltpu.VMEM((sp, 2 * key, span), bf16),
        pltpu.VMEM((heads, pad, key), f32),
        pltpu.VMEM((length, 7 * key), bf16),
        pltpu.VMEM((length + pad, key), f32),
        pltpu.VMEM((length, key), f32),
        pltpu.VMEM((length // BLOCK, key + pad, key), f32),
        pltpu.VMEM((key + 2 * pad, key), f32),
        pltpu.VMEM((lines, key + 2 * pad, key), f32),
        pltpu.VMEM((key, key), f32),
        pltpu.VMEM((every, rows, model), bf16),
        pltpu.VMEM((every // 2, rows, model), bf16),
        pltpu.VMEM((2, rows, half), bf16),
        pltpu.VMEM((2, rows, half), bf16),
        pltpu.VMEM((2, rows, half), bf16),
        dma((heads,)), dma((heads,)), dma((heads,)), dma((every,)), dma((lines,)),
        dma((sp,)), dma((sp,)), dma((sp,)), dma((sp,)),
        dma((sp,)), dma((sp,)), dma((heads,)), dma((every,)), dma((lines,)),
        dma((4,)), dma((4,)), dma((4,)), dma((4,)), dma((2,)), dma((2,)),
        dma((heads,)), dma((2,)),
    ]
    hbm = pl.BlockSpec(memory_space=pl.ANY)
    vmem = pl.BlockSpec(memory_space=pltpu.VMEM)
    return pl.pallas_call(
        functools.partial(fused_kernel, heads, lines, groups, BLOCK),
        out_shape=jax.ShapeDtypeStruct((rows, model), bf16),
        in_specs=[hbm, vmem, (hbm,) * 7, hbm, hbm] + [vmem] * 5,
        out_specs=pl.BlockSpec(memory_space=pltpu.VMEM),
        scratch_shapes=scratch,
        compiler_params=pltpu.CompilerParams(
            collective_id=0, has_side_effects=True, vmem_limit_bytes=60 * 1024 * 1024
        ),
        name="mixer",
    )(
        tokens, norm_gain[None], weights, out_rec, out_conv, floor_gap, extra, start_state,
        state_gain[None], conv_taps,
    )


def per_device(sp, tp, *args):
    heads = args[9].shape[0]
    fits = (
        heads == 4 and tp == 2 and sp % heads == 0
        and args[14].shape[1] % 128 == 0
        and args[13].shape[1] == heads * args[9].shape[1]
        and args[10].shape[0] % BLOCK == 0
    )
    if not fits:
        return on_device(*args)
    return fused(heads, sp // heads, tp, *args)


def solution(mesh):
    placed = (
        P(("sp", "tp"), None),
        P(),
        P("sp", "tp"),
        P("sp", "tp"),
        P("sp", "tp"),
        P("sp", "tp"),
        P("sp", "tp"),
        P("sp", "tp"),
        P("sp", "tp"),
        P("tp", None),
        P("sp", "tp"),
        P("tp", None, None),
        P(),
        P(None, "tp"),
        P("tp", "sp"),
        P("tp", "sp"),
    )
    return jax.shard_map(
        functools.partial(per_device, mesh.shape["sp"], mesh.shape["tp"]), mesh=mesh, in_specs=placed, out_specs=P(("sp", "tp"), None), check_vma=False
    )
```
